32 devices in a mesh: ep: 4 (over y, x), tp: 8 (over z, core).
Axes of the slice: x: 2, y: 2, z: 4, core: 2. Of those that a mesh axis runs over, the one named last changes fastest.
Arguments:
- tokens: bfloat16 [8192, 2048], P(('ep', 'tp')), may hold values from -6 to 6
- norm_gain: float32 [2048], replicated, may hold values from 0.1 to 1.9
- expert_ids: int32 [8192, 2], P(('ep', 'tp')), may hold values from 0 to 3, all different within a row; in each aligned block of 256 rows (0 to 255, 256 to 511, ...) at most 256 rows name the same one
- gate_weights: float32 [8192, 2], P(('ep', 'tp')), may hold values from 0.2 to 1
- w_gate: bfloat16 [4, 2048, 1024], P('ep', None, 'tp'), may hold values from -0.125 to 0.125
- w_up: bfloat16 [4, 2048, 1024], P('ep', None, 'tp'), may hold values from -0.125 to 0.125
- w_down: bfloat16 [4, 2048, 1024], P('ep', None, 'tp'), may hold values from -0.1875 to 0.1875
- dense_gate: bfloat16 [2048, 256], P('ep'), may hold values from -0.125 to 0.125
- dense_up: bfloat16 [2048, 256], P('ep'), may hold values from -0.125 to 0.125
- dense_down: bfloat16 [256, 2048], P(None, 'ep'), may hold values from -0.375 to 0.375
- mix_vector: float32 [2048], replicated, may hold values from -0.125 to 0.125
Outputs:
- mixed: bfloat16 [8192, 2048], P(('ep', 'tp'))
The draws below stay inside these ranges and needn't reach their ends.
Inputs may be any that keep to these rules, and one draw needn't show every extreme that they name: `expert_ids`: A row names 2 different experts. In the rows of one device (aligned blocks of 256 rows) each expert is named by at most 256 rows, a bound that some block reaches.
All inputs are finite; a program needn't handle non-finite values.
Results may differ from the reference program's by a relative error of at most 0.0075.
Values may be sent and summed in bfloat16 or wider, within the bound.
A program may use at most 320 MiB of HBM per device.

```python
import math
import jax
import jax.numpy as jnp
import numpy as np
from jax import lax

D = 2048
FF = 1024
FS = 256
TOPK = 2
TOK_DEV = 256
EXPERTS = 4
CAP = 256
TOKENS = 8192


def steps_of(own_key, shape, pieces, low, largest):
    def one(axis_at, parts):
        heights = jax.random.uniform(jax.random.fold_in(jax.random.fold_in(own_key, 6), axis_at), (parts,), jnp.float32, low / len(pieces), largest / len(pieces))
        return jnp.repeat(jnp.exp(heights), shape[axis_at] // parts).reshape((-1,) + (1,) * (len(shape) - axis_at - 1))

    level = one(*pieces[0])
    for cut in pieces[1:]:
        level = level * one(*cut)
    return level


def shared_out(stream_key, own, number, rows, amount, top, limit, slope):
    order = jax.random.permutation(stream_key, amount)
    crowded, ordinary = load_shares(amount, rows * top, limit, slope, True), load_shares(amount, rows * top, limit, slope, False)
    places = jnp.arange(amount)

    def named(tallies, turn):
        used = int((tallies > 0).sum())
        fixed = max(1, used // 4)
        passed = fixed + (places - fixed + turn * (used - fixed)) % max(1, amount - fixed)
        return jnp.zeros((amount,), jnp.int32).at[order[jnp.where(places < fixed, places, passed)]].set(jnp.asarray(tallies, jnp.int32))

    tallies = jnp.where(number % 4 == 0, named(crowded, number // 4), named(ordinary, number - number // 4 - 1))
    mixed = jax.random.permutation(jax.random.fold_in(own, 3), amount)
    source_of, sink = mixed[0:amount // 2 * 2:2], mixed[1:amount // 2 * 2:2]
    margin = jnp.minimum(tallies[source_of] - 1, limit - tallies[sink]) // 2
    margin = jnp.where((source_of == order[0]) | (sink == order[0]) | (tallies[sink] == 0), 0, jnp.maximum(margin, 0))
    passed = jax.random.randint(jax.random.fold_in(own, 4), (amount // 2,), 0, 1 << 20) % (margin + 1)
    tallies = tallies.at[source_of].add(-passed).at[sink].add(passed)
    labels = jnp.searchsorted(jnp.cumsum(tallies), jnp.arange(rows * top), side="right").astype(jnp.int32)
    table = labels.reshape(top, rows).T
    table = table[jax.random.permutation(jax.random.fold_in(own, 1), rows)]
    turn = jax.random.randint(jax.random.fold_in(own, 2), (rows, 1), 0, top)
    return jnp.take_along_axis(table, (jnp.arange(top)[None, :] + turn) % top, axis=1)


def load_shares(amount, total, bound, slope, full):
    portions = [(1 << 20) // math.isqrt(standing ** slope) + 1 for standing in range(1, amount + 1)]
    largest = bound if full else min(bound, max(-(-total // amount), total * portions[0] // sum(portions)))
    least = 1 if total - largest >= amount - 1 else 0
    counts, surplus = [largest] + [least] * (amount - 1), total - largest - least * (amount - 1)
    while surplus > 0:
        free = [i for i in range(1, amount) if counts[i] < largest] or [i for i in range(1, amount) if counts[i] < bound]
        pool, left = sum([portions[i] for i in free]), surplus
        for i in free:
            addition = min(bound - counts[i], max(1, left * portions[i] // pool), surplus)
            counts[i] = counts[i] + addition
            surplus = surplus - addition
    return np.array(counts)


def normal_values(rng, extent, spread, limit, pieces=(), held_as=jnp.bfloat16):
    values = spread * jax.random.normal(rng, extent, jnp.float32)
    if pieces:
        values = values * steps_of(rng, extent, pieces, -0.22, 0.18)
    return jnp.clip(values, -limit, limit).astype(held_as)


def setup_inputs(seed: int = 0) -> dict:
    keys = jax.random.split(jax.random.key(seed), 12)
    tokens = normal_values(keys[0], (TOKENS, D), 1.0, 6.0, ((0, 32),))
    norm_gain = jnp.clip(1.0 + 0.18 * jax.random.normal(keys[1], (D,), jnp.float32), 0.1, 1.9)
    expert_ids_keys = jax.random.split(jax.random.fold_in(keys[2], 1), TOKENS // TOK_DEV)
    expert_ids_turns = jax.random.permutation(jax.random.fold_in(keys[2], 3), TOKENS // TOK_DEV)
    expert_ids = jax.vmap(lambda own, number: shared_out(jax.random.fold_in(keys[2], 2), own, number, TOK_DEV, EXPERTS, TOPK, CAP, 2))(expert_ids_keys, expert_ids_turns).reshape((TOKENS, TOPK))
    gate_weights = jnp.clip(0.2 + 0.8 * jax.random.uniform(keys[3], (TOKENS, TOPK), jnp.float32) ** steps_of(keys[3], (TOKENS, TOPK), ((0, 32),), -0.2, 0.2), 0.2, 1.0)
    w_gate = normal_values(keys[4], (EXPERTS, D, FF), D ** -0.5, 0.125, ((0, 4), (2, 8)))
    w_up = normal_values(keys[5], (EXPERTS, D, FF), D ** -0.5, 0.125, ((0, 4), (2, 8)))
    w_down = normal_values(keys[6], (EXPERTS, D, FF), FF ** -0.5, 0.1875, ((0, 4), (2, 8)))
    dense_gate = normal_values(keys[7], (D, FS), D ** -0.5, 0.125, ((0, 4),))
    dense_up = normal_values(keys[8], (D, FS), D ** -0.5, 0.125, ((0, 4),))
    dense_down = normal_values(keys[9], (FS, D), FS ** -0.5, 0.375, ((1, 4),))
    mix_vector = normal_values(keys[10], (D,), D ** -0.5, 0.125, (), jnp.float32)
    return dict(tokens=tokens, norm_gain=norm_gain, expert_ids=expert_ids, gate_weights=gate_weights, w_gate=w_gate, w_up=w_up, w_down=w_down, dense_gate=dense_gate, dense_up=dense_up, dense_down=dense_down, mix_vector=mix_vector)


eps = 1e-06

def reference(tokens, norm_gain, expert_ids, gate_weights, w_gate, w_up, w_down, dense_gate, dense_up, dense_down, mix_vector):
    values = tokens.astype(jnp.float32)
    scale = lax.rsqrt(lax.optimization_barrier(jnp.mean(values * values, axis=1, keepdims=True)) + eps)
    normed = (values * scale * norm_gain).astype(jnp.bfloat16)
    blocks = TOKENS // TOK_DEV
    pairs = TOK_DEV * TOPK
    ids = expert_ids.reshape(blocks, pairs)
    onehot = (ids[:, :, None] == jnp.arange(EXPERTS, dtype=jnp.int32)[None, None, :]).astype(jnp.int32)
    before = jnp.cumsum(onehot, axis=1) - onehot
    slot = lax.optimization_barrier(jnp.sum(before * onehot, axis=2)).astype(jnp.int32)
    dest = (ids * CAP + slot).astype(jnp.int32)
    block_rows = jnp.arange(blocks, dtype=jnp.int32)[:, None]
    token_index = block_rows * TOK_DEV + (jnp.arange(pairs, dtype=jnp.int32) // TOPK)[None, :]
    table = jnp.full((blocks, EXPERTS * CAP), TOKENS, jnp.int32)
    table = table.at[block_rows, dest].set(token_index.astype(jnp.int32))
    weight_table = jnp.zeros((blocks, EXPERTS * CAP), jnp.float32)
    weight_table = weight_table.at[block_rows, dest].set(gate_weights.reshape(blocks, pairs))
    padded = jnp.concatenate([normed, jnp.zeros((1, D), jnp.bfloat16)], axis=0)

    def one_expert(total, expert):
        index = lax.dynamic_slice_in_dim(table, (expert * CAP).astype(jnp.int32), CAP, 1).reshape(-1)
        weight = lax.dynamic_slice_in_dim(weight_table, (expert * CAP).astype(jnp.int32), CAP, 1).reshape(-1)
        rows = padded[index]
        gate = jnp.dot(rows, w_gate[expert], preferred_element_type=jnp.float32)
        upper = jnp.dot(rows, w_up[expert], preferred_element_type=jnp.float32)
        hidden = (jax.nn.silu(gate) * upper).astype(jnp.bfloat16)
        result = jnp.dot(hidden, w_down[expert].T, preferred_element_type=jnp.float32).astype(jnp.bfloat16)
        return (total.at[index].add(weight[:, None] * result.astype(jnp.float32)), None)
    start = jnp.zeros((TOKENS + 1, D), jnp.float32)
    routed, unused = lax.scan(one_expert, start, jnp.arange(EXPERTS, dtype=jnp.int32))
    routed = routed[:TOKENS]
    dense_g = jnp.dot(normed, dense_gate, preferred_element_type=jnp.float32)
    dense_u = jnp.dot(normed, dense_up, preferred_element_type=jnp.float32)
    dense_hidden = (jax.nn.silu(dense_g) * dense_u).astype(jnp.bfloat16)
    dense_out = jnp.dot(dense_hidden, dense_down, preferred_element_type=jnp.float32)
    mix = jax.nn.sigmoid(lax.optimization_barrier(jnp.sum(normed.astype(jnp.float32) * mix_vector, axis=1)))
    return (routed + mix[:, None] * dense_out).astype(jnp.bfloat16)
```

```python
import functools

import jax
import jax.numpy as jnp
from jax import lax
from jax.experimental import pallas as pl
from jax.experimental.pallas import tpu as pltpu
from jax.sharding import PartitionSpec as P

MESH = pl.DeviceIdType.MESH
VMEM_BYTES = 65000 * 1024
CORES = 2
PIECES = 3


def moe_kernel(
    ne, nz, x_hbm, wg_hbm, wu_hbm, wd_hbm, dg_hbm, du_hbm, dd_hbm, gw_ref, mix_ref, out_ref,
    xg, ws, dgs, dus, dds, acc, hbuf, ysend, yrecv, side,
    lsem, wrecv, wright, wleft, wpartner, tsend, trecv, dsend, drecv, rsend, rrecv,
):
    me = lax.axis_index("ep")
    tp = lax.axis_index("tp")
    z = tp // CORES
    c = tp % CORES
    rows, width = xg.shape[1], xg.shape[2]
    peers = [(me + k) % ne for k in range(1, ne)]
    partner = z * CORES + (1 - c)

    local = [pltpu.make_async_copy(x_hbm, xg.at[me], lsem.at[0])]
    for p, ref in enumerate((wg_hbm, wu_hbm, wd_hbm)):
        local.append(pltpu.make_async_copy(ref, ws.at[z, c, p], lsem.at[1 + p]))
    for p, (ref, slot) in enumerate(((dg_hbm, dgs), (du_hbm, dus), (dd_hbm, dds))):
        local.append(pltpu.make_async_copy(ref, slot.at[me], lsem.at[4 + p]))
    for copy in local:
        copy.start()

    barrier = pltpu.get_barrier_semaphore()
    for peer in peers:
        pl.semaphore_signal(barrier, inc=1, device_id={"ep": peer}, device_id_type=MESH)
    pl.semaphore_signal(barrier, inc=1, device_id={"tp": partner}, device_id_type=MESH)

    @pl.when(z > 0)
    def _():
        pl.semaphore_signal(barrier, inc=1, device_id={"tp": tp - CORES}, device_id_type=MESH)

    @pl.when(z < nz - 1)
    def _():
        pl.semaphore_signal(barrier, inc=1, device_id={"tp": tp + CORES}, device_id_type=MESH)

    neighbours = (z + nz - 1) // nz + (2 * nz - 2 - z) // nz
    pl.semaphore_wait(barrier, ne + neighbours)

    def weight_copy(src, p, target, sems):
        return pltpu.make_async_remote_copy(
            src_ref=ws.at[src, c, p], dst_ref=ws.at[src, c, p],
            send_sem=sems.at[src, p], recv_sem=wrecv.at[src, c, p],
            device_id={"tp": target}, device_id_type=MESH,
        )

    def to_right(src, p):
        return weight_copy(src, p, tp + CORES, wright)

    def to_left(src, p):
        return weight_copy(src, p, tp - CORES, wleft)

    def to_partner(src, p):
        return weight_copy(src, p, partner, wpartner)

    def await_piece(src, color, p):
        pltpu.make_async_remote_copy(
            src_ref=ws.at[src, color, p], dst_ref=ws.at[src, color, p],
            send_sem=wpartner.at[src, p], recv_sem=wrecv.at[src, color, p],
            device_id={"tp": partner}, device_id_type=MESH,
        ).wait_recv()

    def token_copy(k, block):
        return pltpu.make_async_remote_copy(
            src_ref=xg.at[block], dst_ref=xg.at[block],
            send_sem=tsend.at[k], recv_sem=trecv.at[block],
            device_id={"ep": peers[k]}, device_id_type=MESH,
        )

    def dense_copy(k, p, block):
        slot = (dgs, dus, dds)[p]
        return pltpu.make_async_remote_copy(
            src_ref=slot.at[block], dst_ref=slot.at[block],
            send_sem=dsend.at[k, p], recv_sem=drecv.at[block, p],
            device_id={"ep": peers[k]}, device_id_type=MESH,
        )

    for p in range(PIECES):
        local[1 + p].wait()

        @pl.when(z < nz - 1)
        def _():
            to_right(z, p).start()

        @pl.when(z > 0)
        def _():
            to_left(z, p).start()

        to_partner(z, p).start()
    local[0].wait()
    for k in range(ne - 1):
        token_copy(k, me).start()

    def forward(d, p):
        @pl.when(z >= d)
        def _():
            await_piece(z - d, c, p)

            @pl.when(z < nz - 1)
            def _():
                to_right(z - d, p).start()

            to_partner(z - d, p).start()

        @pl.when(z + d < nz)
        def _():
            await_piece(z + d, c, p)

            @pl.when(z > 0)
            def _():
                to_left(z + d, p).start()

            to_partner(z + d, p).start()

    def hidden(src):
        await_piece(src, 1 - c, 0)
        await_piece(src, 1 - c, 1)

        def one(b, carry):
            x = xg[b]
            wg = jnp.concatenate([ws[src, i, 0] for i in range(CORES)], axis=1)
            g = jnp.dot(x, wg, preferred_element_type=jnp.float32)
            wu = jnp.concatenate([ws[src, i, 1] for i in range(CORES)], axis=1)
            u = jnp.dot(x, wu, preferred_element_type=jnp.float32)
            hbuf[src, b] = (g / (1.0 + jnp.exp(-g)) * u).astype(jnp.bfloat16)
            return carry

        lax.fori_loop(0, ne, one, 0)

    step = 512

    def down(src, first):
        await_piece(src, 1 - c, 2)

        def one(b, carry):
            h = hbuf[src, b]
            for j in range(0, width, step):
                w = jnp.concatenate([ws[src, i, 2, j : j + step, :] for i in range(CORES)], axis=1)
                y = lax.dot_general(
                    h, w, (((1,), (1,)), ((), ())), preferred_element_type=jnp.float32
                )
                if first:
                    acc[b, :, j : j + step] = y
                else:
                    acc[b, :, j : j + step] += y
            return carry

        lax.fori_loop(0, ne, one, 0)

    def both(d, fn):
        @pl.when(z >= d)
        def _():
            fn(z - d)

        @pl.when(z + d < nz)
        def _():
            fn(z + d)

    if nz > 1:
        for p in range(PIECES):
            forward(1, p)
    for p in range(3):
        local[4 + p].wait()
    for k in range(ne - 1):
        block = peers[k]
        token_copy(k, block).wait_recv()
    for p in range(PIECES):
        for k in range(ne - 1):
            dense_copy(k, p, me).start()
    hidden(z)
    down(z, True)
    for d in range(2, nz):
        forward(d, 0)
        both(d - 1, hidden)
        forward(d, 1)
        both(d - 1, lambda src: down(src, False))
        if d == nz - 1:
            both(d, hidden)
        forward(d, 2)
        if d == 2:
            dense_side(ne, me, peers, dense_copy, xg, dgs, dus, dds, mix_ref, side)
    if nz == 2:
        both(1, hidden)
    if nz > 1:
        both(nz - 1, lambda src: down(src, False))

    def back_copy(b, k):
        return pltpu.make_async_remote_copy(
            src_ref=ysend.at[b], dst_ref=yrecv.at[me],
            send_sem=rsend.at[k], recv_sem=rrecv.at[me],
            device_id={"ep": b}, device_id_type=MESH,
        )

    def back_wait(s):
        pltpu.make_async_remote_copy(
            src_ref=ysend.at[s], dst_ref=yrecv.at[s],
            send_sem=rsend.at[0], recv_sem=rrecv.at[s],
            device_id={"ep": s}, device_id_type=MESH,
        ).wait_recv()

    for k in range(ne):
        b = (2 * ne - 1 - me + k) % ne

        @pl.when(b != me)
        def _():
            ysend[b] = acc[b].astype(jnp.bfloat16)
            back_copy(b, k).start()

    yrecv[me] = acc[me].astype(jnp.bfloat16)

    for k in range(ne - 1):
        token_copy(k, me).wait_send()
        for p in range(PIECES):
            dense_copy(k, p, me).wait_send()

    for src in range(nz):
        for p in range(PIECES):
            @pl.when((z < nz - 1) & (z >= src))
            def _():
                to_right(src, p).wait_send()

            @pl.when((z > 0) & (z <= src))
            def _():
                to_left(src, p).wait_send()

            to_partner(src, p).wait_send()

    for k in range(ne):
        b = (2 * ne - 1 - me + k) % ne

        @pl.when(b != me)
        def _():
            back_copy(b, k).wait_send()
            back_wait(b)

    tile = 32

    def combine(i, carry):
        at = pl.ds(pl.multiple_of(i * tile, tile), tile)
        weights = gw_ref[at, :]
        total = side[at, :]
        for s in range(ne):
            total = total + weights[:, s : s + 1] * yrecv[s, at, :].astype(jnp.float32)
        out_ref[at, :] = total.astype(jnp.bfloat16)
        return carry

    lax.fori_loop(0, rows // tile, combine, 0)


def dense_side(ne, me, peers, dense_copy, xg, dgs, dus, dds, mix_ref, side):
    for k in range(ne - 1):
        for p in range(PIECES):
            dense_copy(k, p, peers[k]).wait_recv()
    deep, wide = dgs.shape[1], dds.shape[2]
    g = u = None
    for e in range(ne):
        x = xg[me, :, e * deep : (e + 1) * deep]
        ge = jnp.dot(x, dgs[e], preferred_element_type=jnp.float32)
        ue = jnp.dot(x, dus[e], preferred_element_type=jnp.float32)
        g, u = (ge, ue) if e == 0 else (g + ge, u + ue)
    h = (g / (1.0 + jnp.exp(-g)) * u).astype(jnp.bfloat16)
    for e in range(ne):
        o = jnp.dot(h, dds[e], preferred_element_type=jnp.float32)
        side[:, e * wide : (e + 1) * wide] = mix_ref[...] * o


def fused_layer(ne, tp, normed, gw, mix, w_gate, w_up, w_down, dense_gate, dense_up, dense_down):
    nz = tp // CORES
    rows, width = normed.shape
    shard = w_gate.shape[2]
    bf, f32 = jnp.bfloat16, jnp.float32
    dma = pltpu.SemaphoreType.DMA
    hbm = pl.BlockSpec(memory_space=pl.ANY)
    vmem = pl.BlockSpec(memory_space=pltpu.VMEM)
    flops = 6 * ne * rows * width * shard * tp
    return pl.pallas_call(
        functools.partial(moe_kernel, ne, nz),
        out_shape=jax.ShapeDtypeStruct((rows, width), bf),
        in_specs=[hbm] * 7 + [vmem] * 2,
        out_specs=vmem,
        scratch_shapes=[
            pltpu.VMEM((ne, rows, width), bf),
            pltpu.VMEM((nz, CORES, PIECES, width, shard), bf),
            pltpu.VMEM((ne,) + dense_gate.shape, bf),
            pltpu.VMEM((ne,) + dense_up.shape, bf),
            pltpu.VMEM((ne,) + dense_down.shape, bf),
            pltpu.VMEM((ne, rows, width), f32),
            pltpu.VMEM((nz, ne, rows, CORES * shard), bf),
            pltpu.VMEM((ne, rows, width), bf),
            pltpu.VMEM((ne, rows, width), bf),
            pltpu.VMEM((rows, width), f32),
            dma((7,)),
            dma((nz, CORES, PIECES)),
            dma((nz, PIECES)),
            dma((nz, PIECES)),
            dma((nz, PIECES)),
            dma((ne,)),
            dma((ne,)),
            dma((ne, PIECES)),
            dma((ne, PIECES)),
            dma((ne,)),
            dma((ne,)),
        ],
        compiler_params=pltpu.CompilerParams(
            collective_id=0, has_side_effects=True, vmem_limit_bytes=VMEM_BYTES
        ),
        cost_estimate=pl.CostEstimate(
            flops=flops, bytes_accessed=8 * rows * width, transcendentals=ne * rows * shard * tp
        ),
    )(normed, w_gate[0], w_up[0], w_down[0], dense_gate, dense_up, dense_down, gw, mix)


def fits(ne, tp, tokens, w_gate, dense_gate):
    rows, width = tokens.shape
    shard = w_gate.shape[2]
    block = rows * width
    size = 2 * ne * block * 5 + 8 * block + 2 * PIECES * width * shard * tp
    size += 2 * ne * rows * shard * tp + 6 * ne * dense_gate.size
    aligned = shard % 128 == 0 and width % 512 == 0 and rows % 32 == 0
    return tp % CORES == 0 and tp > CORES and aligned and size < VMEM_BYTES * 15 // 16


eps = 1e-06


def dense_branch(normed, dense_gate, dense_up, dense_down, mix_vector):
    dense_g = jnp.dot(
        normed,
        lax.all_gather(dense_gate, "ep", axis=0, tiled=True),
        preferred_element_type=jnp.float32,
    )
    dense_u = jnp.dot(
        normed,
        lax.all_gather(dense_up, "ep", axis=0, tiled=True),
        preferred_element_type=jnp.float32,
    )
    dense_hidden = (jax.nn.silu(dense_g) * dense_u).astype(jnp.bfloat16)
    dense_out = jnp.dot(
        dense_hidden,
        lax.all_gather(dense_down, "ep", axis=1, tiled=True),
        preferred_element_type=jnp.float32,
    )
    mix = jax.nn.sigmoid(jnp.sum(normed.astype(jnp.float32) * mix_vector, axis=1))
    return mix[:, None] * dense_out


def on_device(
    tokens,
    norm_gain,
    expert_ids,
    gate_weights,
    w_gate,
    w_up,
    w_down,
    dense_gate,
    dense_up,
    dense_down,
    mix_vector,
):
    values = tokens.astype(jnp.float32)
    scale = lax.rsqrt(jnp.mean(values * values, axis=1, keepdims=True) + eps)
    normed = (values * scale * norm_gain).astype(jnp.bfloat16)
    count_tok, topk = expert_ids.shape
    width = tokens.shape[1]
    groups = lax.axis_size("ep")
    ring = lax.axis_size("tp")
    if fits(groups, ring, tokens, w_gate, dense_gate):
        named = expert_ids[:, :, None] == jnp.arange(groups, dtype=jnp.int32)[None, None, :]
        gw = jnp.sum(jnp.where(named, gate_weights[:, :, None], 0.0), axis=1)
        mix = jax.nn.sigmoid(
            jnp.sum(normed.astype(jnp.float32) * mix_vector, axis=1, keepdims=True)
        )
        return fused_layer(
            groups, ring, normed, gw, mix, w_gate, w_up, w_down, dense_gate, dense_up, dense_down
        )
    capacity = 2 * count_tok * topk // groups
    flat_ids = expert_ids.reshape(-1)
    onehot = (flat_ids[:, None] == jnp.arange(groups, dtype=jnp.int32)[None, :]).astype(jnp.int32)
    before = jnp.cumsum(onehot, axis=0) - onehot
    slot = jnp.sum(before * onehot, axis=1)
    dest = flat_ids * capacity + slot
    owner = jnp.arange(count_tok * topk, dtype=jnp.int32) // topk
    buffer = jnp.zeros((groups * capacity, width), jnp.bfloat16).at[dest].set(normed[owner])
    arrived = lax.all_to_all(
        buffer.reshape(groups, capacity, width), "ep", split_axis=0, concat_axis=0, tiled=True
    )
    rows = arrived.reshape(groups * capacity, width)
    gate = jnp.dot(
        rows,
        lax.all_gather(w_gate, "tp", axis=2, tiled=True)[0],
        preferred_element_type=jnp.float32,
    )
    upper = jnp.dot(
        rows, lax.all_gather(w_up, "tp", axis=2, tiled=True)[0], preferred_element_type=jnp.float32
    )
    hidden_all = (jax.nn.silu(gate) * upper).astype(jnp.bfloat16)
    expert_out = lax.dot_general(
        hidden_all,
        lax.all_gather(w_down, "tp", axis=2, tiled=True)[0],
        (((1,), (1,)), ((), ())),
        preferred_element_type=jnp.float32,
    )
    results = expert_out.astype(jnp.bfloat16).reshape(groups, capacity, width)
    returned = lax.all_to_all(results, "ep", split_axis=0, concat_axis=0, tiled=True)
    picked = returned.reshape(groups * capacity, width)[dest].reshape(count_tok, topk, width)
    routed = jnp.einsum("tk,tkd->td", gate_weights, picked.astype(jnp.float32))
    side = dense_branch(normed, dense_gate, dense_up, dense_down, mix_vector)
    return (routed + side).astype(jnp.bfloat16)


def solution(mesh):
    placed = (
        P(("ep", "tp"), None),
        P(),
        P(("ep", "tp"), None),
        P(("ep", "tp"), None),
        P("ep", None, "tp"),
        P("ep", None, "tp"),
        P("ep", None, "tp"),
        P("ep", None),
        P("ep", None),
        P(None, "ep"),
        P(),
    )
    return jax.shard_map(
        on_device, mesh=mesh, in_specs=placed, out_specs=P(("ep", "tp"), None), check_vma=False
    )
```

```python
import functools

import jax
import jax.numpy as jnp
from jax import lax
from jax.experimental import pallas as pl
from jax.experimental.pallas import tpu as pltpu
from jax.sharding import PartitionSpec as P

MESH = pl.DeviceIdType.MESH
VMEM_BYTES = 65000 * 1024
CORES = 2
PIECES = 3
LANES = 128
eps = 1e-06


def moe_kernel(
    ne, nz, x_hbm, wg_hbm, wu_hbm, wd_hbm, dg_hbm, du_hbm, dd_hbm, ids_hbm, gates_hbm,
    gain_ref, mixv_ref, out_ref,
    xg, ws, dgs, dus, dds, acc, hbuf, ysend, yrecv, relay, side, ids, gates, mix_ref, stage, wts,
    lsem, wrecv, wright, wleft, wpartner, tsend, trecv, gsend, grecv, dsend, drecv, rsend, rrecv,
):
    me = lax.axis_index("ep")
    tp = lax.axis_index("tp")
    z = tp // CORES
    c = tp % CORES
    rows, width = xg.shape[1], xg.shape[2]
    peers = [(me + k) % ne for k in range(1, ne)]
    partner = z * CORES + (1 - c)

    local = [pltpu.make_async_copy(x_hbm, ysend.at[1], lsem.at[0])]
    for p, ref in enumerate((wg_hbm, wu_hbm, wd_hbm)):
        local.append(pltpu.make_async_copy(ref, ws.at[z, c, p], lsem.at[1 + p]))
    for p, (ref, slot) in enumerate(((dg_hbm, dgs), (du_hbm, dus), (dd_hbm, dds))):
        local.append(pltpu.make_async_copy(ref, slot.at[me], lsem.at[4 + p]))
    local.append(pltpu.make_async_copy(ids_hbm, ids, lsem.at[7]))
    local.append(pltpu.make_async_copy(gates_hbm, gates, lsem.at[8]))
    for copy in local:
        copy.start()

    barrier = pltpu.get_barrier_semaphore()
    for peer in peers:
        pl.semaphore_signal(barrier, inc=1, device_id={"ep": peer}, device_id_type=MESH)
    pl.semaphore_signal(barrier, inc=1, device_id={"tp": partner}, device_id_type=MESH)

    @pl.when(z > 0)
    def _():
        pl.semaphore_signal(barrier, inc=1, device_id={"tp": tp - CORES}, device_id_type=MESH)

    @pl.when(z < nz - 1)
    def _():
        pl.semaphore_signal(barrier, inc=1, device_id={"tp": tp + CORES}, device_id_type=MESH)

    neighbours = (z + nz - 1) // nz + (2 * nz - 2 - z) // nz
    pl.semaphore_wait(barrier, ne + neighbours)

    def weight_copy(src, p, target, sems):
        return pltpu.make_async_remote_copy(
            src_ref=ws.at[src, c, p], dst_ref=ws.at[src, c, p],
            send_sem=sems.at[src, p], recv_sem=wrecv.at[src, c, p],
            device_id={"tp": target}, device_id_type=MESH,
        )

    def to_right(src, p):
        return weight_copy(src, p, tp + CORES, wright)

    def to_left(src, p):
        return weight_copy(src, p, tp - CORES, wleft)

    def to_partner(src, p):
        return weight_copy(src, p, partner, wpartner)

    def await_piece(src, color, p):
        pltpu.make_async_remote_copy(
            src_ref=ws.at[src, color, p], dst_ref=ws.at[src, color, p],
            send_sem=wpartner.at[src, p], recv_sem=wrecv.at[src, color, p],
            device_id={"tp": partner}, device_id_type=MESH,
        ).wait_recv()

    def token_copy(k, block):
        return pltpu.make_async_remote_copy(
            src_ref=xg.at[block], dst_ref=xg.at[block],
            send_sem=tsend.at[k], recv_sem=trecv.at[block],
            device_id={"ep": peers[k]}, device_id_type=MESH,
        )

    def gate_copy(k, block):
        return pltpu.make_async_remote_copy(
            src_ref=wts.at[block], dst_ref=wts.at[block],
            send_sem=gsend.at[k], recv_sem=grecv.at[block],
            device_id={"ep": peers[k]}, device_id_type=MESH,
        )

    def dense_copy(k, p, block):
        slot = (dgs, dus, dds)[p]
        return pltpu.make_async_remote_copy(
            src_ref=slot.at[block], dst_ref=slot.at[block],
            send_sem=dsend.at[k, p], recv_sem=drecv.at[block, p],
            device_id={"ep": peers[k]}, device_id_type=MESH,
        )

    for p in range(PIECES):
        local[1 + p].wait()

        @pl.when(z < nz - 1)
        def _():
            to_right(z, p).start()

        @pl.when(z > 0)
        def _():
            to_left(z, p).start()

        to_partner(z, p).start()
    for i in (0, 7, 8):
        local[i].wait()
    tile = 32
    lane = lax.broadcasted_iota(jnp.int32, (tile, LANES), 1)

    def norm(i, carry):
        at = pl.ds(pl.multiple_of(i * tile, tile), tile)
        named, gate = ids[at, :], gates[at, :]
        weight = jnp.zeros((tile, LANES), jnp.float32)
        for k in range(named.shape[1]):
            weight += jnp.where(named[:, k : k + 1] == lane, gate[:, k : k + 1], 0.0)
        stage[at, :] = weight
        v = ysend[1, at, :].astype(jnp.float32)
        scale = lax.rsqrt(jnp.sum(v * v, axis=1, keepdims=True) * (1.0 / width) + eps)
        n = (v * scale * gain_ref[...]).astype(jnp.bfloat16)
        ysend[0, at, :] = n
        m = jnp.sum(n.astype(jnp.float32) * mixv_ref[...], axis=1, keepdims=True)
        mix_ref[at, :] = 1.0 / (1.0 + jnp.exp(-m))
        return carry

    lax.fori_loop(0, rows // tile, norm, 0)
    staged = [
        pltpu.make_async_copy(ysend.at[0], xg.at[me], lsem.at[9]),
        pltpu.make_async_copy(stage, wts.at[me], lsem.at[10]),
    ]
    for copy in staged:
        copy.start()
    for copy in staged:
        copy.wait()
    for k in range(ne - 1):
        token_copy(k, me).start()
    for k in range(ne - 1):
        gate_copy(k, me).start()

    def forward(d, p):
        @pl.when(z >= d)
        def _():
            await_piece(z - d, c, p)

            @pl.when(z < nz - 1)
            def _():
                to_right(z - d, p).start()

            to_partner(z - d, p).start()

        @pl.when(z + d < nz)
        def _():
            await_piece(z + d, c, p)

            @pl.when(z > 0)
            def _():
                to_left(z + d, p).start()

            to_partner(z + d, p).start()

    def hidden(src):
        await_piece(src, 1 - c, 0)
        await_piece(src, 1 - c, 1)

        def one(b, carry):
            x = xg[b]
            wg = jnp.concatenate([ws[src, i, 0] for i in range(CORES)], axis=1)
            g = jnp.dot(x, wg, preferred_element_type=jnp.float32)
            wu = jnp.concatenate([ws[src, i, 1] for i in range(CORES)], axis=1)
            u = jnp.dot(x, wu, preferred_element_type=jnp.float32)
            hbuf[src, b] = (g / (1.0 + jnp.exp(-g)) * u).astype(jnp.bfloat16)
            return carry

        lax.fori_loop(0, ne, one, 0)

    step = 512

    def down_block(src, b, first):
        h = hbuf[src, b]
        for j in range(0, width, step):
            w = jnp.concatenate([ws[src, i, 2, j : j + step, :] for i in range(CORES)], axis=1)
            y = lax.dot_general(
                h, w, (((1,), (1,)), ((), ())), preferred_element_type=jnp.float32
            )
            if first:
                acc[b, :, j : j + step] = y
            else:
                acc[b, :, j : j + step] += y

    def down(src, first):
        await_piece(src, 1 - c, 2)

        def one(b, carry):
            down_block(src, b, first)
            return carry

        lax.fori_loop(0, ne, one, 0)

    def both(d, fn):
        @pl.when(z >= d)
        def _():
            fn(z - d)

        @pl.when(z + d < nz)
        def _():
            fn(z + d)

    for p in range(PIECES):
        forward(1, p)
    for p in range(3):
        local[4 + p].wait()
    for k in range(ne - 1):
        token_copy(k, peers[k]).wait_recv()
    for k in range(ne - 1):
        gate_copy(k, peers[k]).wait_recv()
    for p in range(PIECES):
        for k in range(ne - 1):
            dense_copy(k, p, me).start()
    hidden(z)
    down(z, True)
    for d in range(2, nz):
        forward(d, 0)
        both(d - 1, hidden)
        forward(d, 1)
        both(d - 1, lambda src: down(src, False))
        if d == nz - 1:
            both(d, hidden)
        forward(d, 2)
        if d == 2:
            dense_side(ne, me, peers, dense_copy, xg, dgs, dus, dds, mix_ref, side)
    across, along, diagonal = me + 1 - 2 * (me % 2), (me + 2) % ne, ne - 1 - me
    half = rows // 2

    def back(k):
        block = (diagonal, diagonal, across, along, along, across)[k]
        peer = (across, along, across, along, along, across)[k]
        low = (0, half, 0, half, 0, half)[k]
        lands = relay.at[k] if k < 2 else yrecv.at[k % 2 if k < 4 else 1 - k % 2, low : low + half]
        return pltpu.make_async_remote_copy(
            src_ref=ysend.at[block, low : low + half], dst_ref=lands,
            send_sem=rsend.at[k], recv_sem=rrecv.at[k],
            device_id={"ep": peer}, device_id_type=MESH,
        )

    def column(block, at):
        return jnp.sum(jnp.where(lane == me, wts[block, at, :], 0.0), axis=1, keepdims=True)

    def fill(block, low, relayed):
        def one(i, carry):
            at = pl.ds(pl.multiple_of(low + i * tile, tile), tile)
            v = acc[block, at, :] * column(block, at)
            if relayed is not None:
                here = pl.ds(pl.multiple_of(i * tile, tile), tile)
                v += relay[relayed, here, :].astype(jnp.float32)
            ysend[block, at, :] = v.astype(jnp.bfloat16)
            return carry

        lax.fori_loop(0, half // tile, one, 0)

    both(nz - 1, lambda src: await_piece(src, 1 - c, 2))
    both(nz - 1, lambda src: down_block(src, diagonal, False))
    fill(diagonal, 0, None)
    back(0).start()
    fill(diagonal, half, None)
    back(1).start()
    both(nz - 1, lambda src: down_block(src, across, False))
    fill(across, 0, None)
    back(2).start()
    both(nz - 1, lambda src: down_block(src, along, False))
    fill(along, half, None)
    back(3).start()
    both(nz - 1, lambda src: down_block(src, me, False))
    back(0).wait_recv()
    fill(along, 0, 0)
    back(4).start()
    back(1).wait_recv()
    fill(across, half, 1)
    back(5).start()

    for k in range(ne - 1):
        token_copy(k, me).wait_send()
        gate_copy(k, me).wait_send()
        for p in range(PIECES):
            dense_copy(k, p, me).wait_send()

    for src in range(nz):
        for p in range(PIECES):
            @pl.when((z < nz - 1) & (z >= src))
            def _():
                to_right(src, p).wait_send()

            @pl.when((z > 0) & (z <= src))
            def _():
                to_left(src, p).wait_send()

            to_partner(src, p).wait_send()

    for k in range(6):
        back(k).wait_send()
    for k in range(2, 6):
        back(k).wait_recv()

    def combine(i, carry):
        at = pl.ds(pl.multiple_of(i * tile, tile), tile)
        total = side[at, :] + acc[me, at, :] * column(me, at)
        for k in range(2):
            total = total + yrecv[k, at, :].astype(jnp.float32)
        out_ref[at, :] = total.astype(jnp.bfloat16)
        return carry

    lax.fori_loop(0, rows // tile, combine, 0)


def dense_side(ne, me, peers, dense_copy, xg, dgs, dus, dds, mix_ref, side):
    for k in range(ne - 1):
        for p in range(PIECES):
            dense_copy(k, p, peers[k]).wait_recv()
    deep, wide = dgs.shape[1], dds.shape[2]
    g = u = None
    for e in range(ne):
        x = xg[me, :, e * deep : (e + 1) * deep]
        ge = jnp.dot(x, dgs[e], preferred_element_type=jnp.float32)
        ue = jnp.dot(x, dus[e], preferred_element_type=jnp.float32)
        g, u = (ge, ue) if e == 0 else (g + ge, u + ue)
    h = (g / (1.0 + jnp.exp(-g)) * u).astype(jnp.bfloat16)
    for e in range(ne):
        o = jnp.dot(h, dds[e], preferred_element_type=jnp.float32)
        side[:, e * wide : (e + 1) * wide] = mix_ref[...] * o


def fused_layer(
    ne, tp, tokens, norm_gain, expert_ids, gate_weights,
    w_gate, w_up, w_down, dense_gate, dense_up, dense_down, mix_vector,
):
    nz = tp // CORES
    rows, width = tokens.shape
    topk = expert_ids.shape[1]
    shard = w_gate.shape[2]
    bf, f32 = jnp.bfloat16, jnp.float32
    dma = pltpu.SemaphoreType.DMA
    hbm = pl.BlockSpec(memory_space=pl.ANY)
    vmem = pl.BlockSpec(memory_space=pltpu.VMEM)
    flops = 6 * ne * rows * width * shard * tp
    return pl.pallas_call(
        functools.partial(moe_kernel, ne, nz),
        out_shape=jax.ShapeDtypeStruct((rows, width), bf),
        in_specs=[hbm] * 9 + [vmem] * 2,
        out_specs=vmem,
        scratch_shapes=[
            pltpu.VMEM((ne, rows, width), bf),
            pltpu.VMEM((nz, CORES, PIECES, width, shard), bf),
            pltpu.VMEM((ne,) + dense_gate.shape, bf),
            pltpu.VMEM((ne,) + dense_up.shape, bf),
            pltpu.VMEM((ne,) + dense_down.shape, bf),
            pltpu.VMEM((ne, rows, width), f32),
            pltpu.VMEM((nz, ne, rows, CORES * shard), bf),
            pltpu.VMEM((ne, rows, width), bf),
            pltpu.VMEM((2, rows, width), bf),
            pltpu.VMEM((2, rows // 2, width), bf),
            pltpu.VMEM((rows, width), f32),
            pltpu.VMEM((rows, topk), jnp.int32),
            pltpu.VMEM((rows, topk), f32),
            pltpu.VMEM((rows, 1), f32),
            pltpu.VMEM((rows, LANES), f32),
            pltpu.VMEM((ne, rows, LANES), f32),
            dma((11,)),
            dma((nz, CORES, PIECES)),
            dma((nz, PIECES)),
            dma((nz, PIECES)),
            dma((nz, PIECES)),
            dma((ne,)),
            dma((ne,)),
            dma((ne,)),
            dma((ne,)),
            dma((ne, PIECES)),
            dma((ne, PIECES)),
            dma((6,)),
            dma((6,)),
        ],
        compiler_params=pltpu.CompilerParams(
            collective_id=0, has_side_effects=True, vmem_limit_bytes=VMEM_BYTES
        ),
        cost_estimate=pl.CostEstimate(
            flops=flops, bytes_accessed=8 * rows * width, transcendentals=ne * rows * shard * tp
        ),
    )(
        tokens, w_gate[0], w_up[0], w_down[0], dense_gate, dense_up, dense_down,
        expert_ids, gate_weights, norm_gain.reshape(1, width), mix_vector.reshape(1, width),
    )


def fits(ne, tp, tokens, w_gate, dense_gate):
    rows, width = tokens.shape
    shard = w_gate.shape[2]
    block = rows * width
    size = 2 * ne * block * 5 + 8 * block + 2 * PIECES * width * shard * tp
    size += 2 * ne * rows * shard * tp + 6 * ne * dense_gate.size
    aligned = shard % 128 == 0 and width % 512 == 0 and rows % 64 == 0
    return ne == 4 and tp % CORES == 0 and tp > 2 * CORES and aligned and size < VMEM_BYTES * 15 // 16


def dense_branch(normed, dense_gate, dense_up, dense_down, mix_vector):
    dense_g = jnp.dot(
        normed,
        lax.all_gather(dense_gate, "ep", axis=0, tiled=True),
        preferred_element_type=jnp.float32,
    )
    dense_u = jnp.dot(
        normed,
        lax.all_gather(dense_up, "ep", axis=0, tiled=True),
        preferred_element_type=jnp.float32,
    )
    dense_hidden = (jax.nn.silu(dense_g) * dense_u).astype(jnp.bfloat16)
    dense_out = jnp.dot(
        dense_hidden,
        lax.all_gather(dense_down, "ep", axis=1, tiled=True),
        preferred_element_type=jnp.float32,
    )
    mix = jax.nn.sigmoid(jnp.sum(normed.astype(jnp.float32) * mix_vector, axis=1))
    return mix[:, None] * dense_out


def on_device(
    tokens,
    norm_gain,
    expert_ids,
    gate_weights,
    w_gate,
    w_up,
    w_down,
    dense_gate,
    dense_up,
    dense_down,
    mix_vector,
):
    groups = lax.axis_size("ep")
    ring = lax.axis_size("tp")
    if fits(groups, ring, tokens, w_gate, dense_gate):
        return fused_layer(
            groups, ring, tokens, norm_gain, expert_ids, gate_weights,
            w_gate, w_up, w_down, dense_gate, dense_up, dense_down, mix_vector,
        )
    values = tokens.astype(jnp.float32)
    scale = lax.rsqrt(jnp.mean(values * values, axis=1, keepdims=True) + eps)
    normed = (values * scale * norm_gain).astype(jnp.bfloat16)
    count_tok, topk = expert_ids.shape
    width = tokens.shape[1]
    capacity = 2 * count_tok * topk // groups
    flat_ids = expert_ids.reshape(-1)
    onehot = (flat_ids[:, None] == jnp.arange(groups, dtype=jnp.int32)[None, :]).astype(jnp.int32)
    before = jnp.cumsum(onehot, axis=0) - onehot
    slot = jnp.sum(before * onehot, axis=1)
    dest = flat_ids * capacity + slot
    owner = jnp.arange(count_tok * topk, dtype=jnp.int32) // topk
    buffer = jnp.zeros((groups * capacity, width), jnp.bfloat16).at[dest].set(normed[owner])
    arrived = lax.all_to_all(
        buffer.reshape(groups, capacity, width), "ep", split_axis=0, concat_axis=0, tiled=True
    )
    rows = arrived.reshape(groups * capacity, width)
    gate = jnp.dot(
        rows,
        lax.all_gather(w_gate, "tp", axis=2, tiled=True)[0],
        preferred_element_type=jnp.float32,
    )
    upper = jnp.dot(
        rows, lax.all_gather(w_up, "tp", axis=2, tiled=True)[0], preferred_element_type=jnp.float32
    )
    hidden_all = (jax.nn.silu(gate) * upper).astype(jnp.bfloat16)
    expert_out = lax.dot_general(
        hidden_all,
        lax.all_gather(w_down, "tp", axis=2, tiled=True)[0],
        (((1,), (1,)), ((), ())),
        preferred_element_type=jnp.float32,
    )
    results = expert_out.astype(jnp.bfloat16).reshape(groups, capacity, width)
    returned = lax.all_to_all(results, "ep", split_axis=0, concat_axis=0, tiled=True)
    picked = returned.reshape(groups * capacity, width)[dest].reshape(count_tok, topk, width)
    routed = jnp.einsum("tk,tkd->td", gate_weights, picked.astype(jnp.float32))
    side = dense_branch(normed, dense_gate, dense_up, dense_down, mix_vector)
    return (routed + side).astype(jnp.bfloat16)


def solution(mesh):
    placed = (
        P(("ep", "tp"), None),
        P(),
        P(("ep", "tp"), None),
        P(("ep", "tp"), None),
        P("ep", None, "tp"),
        P("ep", None, "tp"),
        P("ep", None, "tp"),
        P("ep", None),
        P("ep", None),
        P(None, "ep"),
        P(),
    )
    return jax.shard_map(
        on_device, mesh=mesh, in_specs=placed, out_specs=P(("ep", "tp"), None), check_vma=False
    )
```
